32 devices in a mesh: grp: 2 (over y), fs: 4 (over z), tp: 4 (over x, core).
Axes of the slice: x: 2, y: 2, z: 4, core: 2. Of those that a mesh axis runs over, the one named last changes fastest.
Arguments:
- stream: bfloat16 [8, 128, 2048], P(('grp', 'fs')), parts along dimension 0, may hold values from -6 to 6
- in_gain: float32 [2048], replicated, may hold values from 0.2 to 5
- value_weight: bfloat16 [2048, 1024], P('fs', 'tp'), may hold values from -0.125 to 0.125
- gate_weight: bfloat16 [2048, 1024], P('fs', 'tp'), may hold values from -0.125 to 0.125
- conv_kernel: bfloat16 [31, 1024], P(None, 'tp'), may hold values from -3.6 to 3.6
- conv_gain: float32 [1024], P('tp'), may hold values from 0.1 to 1.9
- conv_shift: float32 [1024], P('tp'), may hold values from -3 to 3
- out_weight: bfloat16 [1024, 2048], P('tp', 'fs'), may hold values from -0.1875 to 0.1875
- norm_gain: float32 [2048], replicated, may hold values from 0.2 to 5
- up_weight: bfloat16 [2048, 8192], P('fs', 'tp'), may hold values from -0.125 to 0.125
- down_weight: bfloat16 [8192, 2048], P('tp', 'fs'), may hold values from -0.0625 to 0.0625
- out_gain: float32 [2048], P('tp'), may hold values from 0.1 to 1.9
Outputs:
- result: bfloat16 [8, 128, 2048], P(('grp', 'fs'), None, 'tp'), parts along dimension 0
The draws below stay inside these ranges and needn't reach their ends.
There are 2 independent parts, one for each index of `grp`. The reference program is written for one: setup_inputs(seed, part) draws one part's arguments, and reference() takes and returns one part's arrays. A program takes and returns all parts, laid end to end along the dimension named above; an argument that names none is the same for every part. Nothing has to cross between parts.
All inputs are finite; a program needn't handle non-finite values.
Results may differ from the reference program's by a relative error of at most 0.02.
Values may be sent and summed in bfloat16 or wider, within the bound.
A program may use at most 64 MiB of HBM per device.

```python
import jax
import jax.numpy as jnp
from jax import lax

D = 2048
DC = 1024
FF = 8192
KW = 31
SEQ_LEN = 128
SEQS = 4
N_TP = 4


def rising(key, length_count, span):
    spread_at = jnp.arange(length_count, dtype=jnp.float32) / (length_count - 1) * 2.0 - 1.0
    baseline = 10.0 ** (span * spread_at)
    roughness = jax.random.uniform(key, (length_count,), jnp.float32, 0.8, 1.25)
    return baseline * roughness


def draw_in_gain(key, part):
    return rising(jax.random.fold_in(key, 11), D, 0.45).astype(jnp.float32)


def draw_norm_gain(key, part):
    return rising(jax.random.fold_in(key, 23), D, 0.45).astype(jnp.float32)


def draw_conv_kernel(key, part):
    inner = jax.random.fold_in(key, 37)
    taps = jnp.clip(jax.random.normal(inner, (KW, DC), jnp.float32), -4.0, 4.0)
    scales = rising(jax.random.fold_in(key, 41), DC, 0.45)
    return (taps * KW ** (-0.5) * scales[None, :]).astype(jnp.bfloat16)


def block_levels(rng, extent, cuts, least, top_value):
    loudness, own = 1.0, jax.random.fold_in(rng, 6)
    for position, parts in cuts:
        heights = jnp.exp(jax.random.uniform(jax.random.fold_in(own, position), (parts,), jnp.float32, least / len(cuts), top_value / len(cuts)))
        loudness = loudness * jnp.repeat(heights, extent[position] // parts).reshape([-1 if axis == position else 1 for axis in range(len(extent))])
    return loudness


def gaussian(key, extent, deviation, limit, pieces=(), held_as=jnp.bfloat16):
    values = jax.random.normal(key, extent, jnp.float32) * deviation
    if len(pieces) > 0:
        values = block_levels(key, extent, pieces, -0.22, 0.18) * values
    return jnp.clip(values, min=-limit, max=limit).astype(held_as)


def setup_inputs(seed: int = 0, part: int = 0) -> dict:
    streams_of = jax.random.split(jax.random.key(seed), 13)
    part_keys = jax.random.split(jax.random.fold_in(streams_of[12], part), 13)
    return {
        "stream": gaussian(part_keys[0], (SEQS, SEQ_LEN, D), 1.0, 6.0, ((0, 4),)),
        "in_gain": draw_in_gain(jax.random.fold_in(streams_of[12], 71), part),
        "value_weight": gaussian(streams_of[2], (D, DC), D ** -0.5, 0.125, ((0, 4), (1, 4))),
        "gate_weight": gaussian(streams_of[3], (D, DC), D ** -0.5, 0.125, ((0, 4), (1, 4))),
        "conv_kernel": draw_conv_kernel(jax.random.fold_in(streams_of[12], 71), part),
        "conv_gain": jnp.clip(1.0 + 0.18 * jax.random.normal(streams_of[5], (DC,), jnp.float32), 0.1, 1.9),
        "conv_shift": gaussian(streams_of[6], (DC,), 0.5, 3.0, ((0, 4),), jnp.float32),
        "out_weight": gaussian(streams_of[7], (DC, D), DC ** -0.5, 0.1875, ((0, 4), (1, 4))),
        "norm_gain": draw_norm_gain(jax.random.fold_in(streams_of[12], 71), part),
        "up_weight": gaussian(streams_of[9], (D, FF), D ** -0.5, 0.125, ((0, 4), (1, 4))),
        "down_weight": gaussian(streams_of[10], (FF, D), FF ** -0.5, 0.0625, ((0, 4), (1, 4))),
        "out_gain": jnp.clip(1.0 + 0.18 * jax.random.normal(streams_of[11], (D,), jnp.float32), 0.1, 1.9),
    }


norm_epsilon = 1e-05
residual_scale = 2.0 ** 0.25

def layer_norm(values, gain_vector):
    row_mean = lax.optimization_barrier(jnp.mean(values, axis=-1, keepdims=True))
    row_var = lax.optimization_barrier(jnp.mean(jnp.square(values - row_mean), axis=-1, keepdims=True))
    return (values - row_mean) * lax.rsqrt(row_var + norm_epsilon) * gain_vector

def grouped_product(left, right, groups):
    width = left.shape[1] // groups
    accum = jnp.zeros((left.shape[0], right.shape[1]), jnp.float32)
    for group_index in range(groups):
        partial_value = jnp.dot(left[:, group_index * width:(group_index + 1) * width], right[group_index * width:(group_index + 1) * width], preferred_element_type=jnp.float32).astype(jnp.bfloat16)
        partial_value = lax.optimization_barrier(partial_value)
        accum = accum + partial_value.astype(jnp.float32)
    return accum.astype(jnp.bfloat16)

def reference(stream, in_gain, value_weight, gate_weight, conv_kernel, conv_gain, conv_shift, out_weight, norm_gain, up_weight, down_weight, out_gain):
    seq_count, seq_length, model_width = stream.shape
    token_count = seq_count * seq_length
    stream_rows = stream.reshape(token_count, model_width).astype(jnp.float32)
    normed = layer_norm(stream_rows, in_gain).astype(jnp.bfloat16)
    values = jnp.dot(normed, value_weight, preferred_element_type=jnp.float32)
    gating = jnp.dot(normed, gate_weight, preferred_element_type=jnp.float32)
    gated = (values * jax.nn.sigmoid(gating)).astype(jnp.bfloat16)
    channels = gated.shape[1]
    convolved = lax.conv_general_dilated(gated.reshape(seq_count, seq_length, channels), conv_kernel[:, None, :], window_strides=(1,), padding=[(KW - 1, 0)], dimension_numbers=('NWC', 'WIO', 'NWC'), feature_group_count=channels, preferred_element_type=jnp.float32).reshape(token_count, channels)
    activated = jax.nn.silu(layer_norm(convolved, conv_gain) + conv_shift).astype(jnp.bfloat16)
    mixed = grouped_product(activated, out_weight, N_TP)
    settled = layer_norm(residual_scale * normed.astype(jnp.float32) + mixed.astype(jnp.float32), norm_gain).astype(jnp.bfloat16)
    hidden = jnp.square(jax.nn.relu(jnp.dot(settled, up_weight, preferred_element_type=jnp.float32))).astype(jnp.bfloat16)
    fed = grouped_product(hidden, down_weight, N_TP)
    result = layer_norm(residual_scale * settled.astype(jnp.float32) + fed.astype(jnp.float32), out_gain)
    return result.astype(jnp.bfloat16).reshape(seq_count, seq_length, model_width)
```

```python
import functools

import jax
import jax.numpy as jnp
from jax import lax
from jax.experimental import pallas as pl
from jax.experimental.pallas import tpu as pltpu
from jax.sharding import PartitionSpec as P

KW = 31


norm_epsilon = 1e-05
residual_scale = 2.0**0.25


def norm_rows(values, gain_vector):
    row_mean = jnp.mean(values, axis=-1, keepdims=True)
    row_var = jnp.mean(jnp.square(values - row_mean), axis=-1, keepdims=True)
    return (values - row_mean) * lax.rsqrt(row_var + norm_epsilon) * gain_vector


def norm_shares(summed, stat_sums, full_width, gain_vector):
    row_mean = stat_sums[0] / full_width
    row_var = stat_sums[1] / full_width - row_mean * row_mean
    return (summed - row_mean[:, None]) * lax.rsqrt(row_var + norm_epsilon)[:, None] * gain_vector


def row_sums(summed):
    return (jnp.sum(summed, axis=1), jnp.sum(summed * summed, axis=1))


def contract(left, turned):
    return lax.dot_general(
        left, turned, (((1,), (1,)), ((), ())), preferred_element_type=jnp.float32
    )


def shards(
    stream,
    in_gain,
    value_weight,
    gate_weight,
    conv_kernel,
    conv_gain,
    conv_shift,
    out_weight,
    norm_gain,
    up_weight,
    down_weight,
    out_gain,
):
    seq_count, seq_length, model_width = stream.shape
    token_count = seq_count * seq_length
    tp_count = lax.axis_size("tp")
    slice_width = model_width // tp_count
    tp_index = lax.axis_index("tp")
    out_turned_shard = out_weight.T
    down_turned_shard = down_weight.T
    value_whole, gate_whole, out_turned, up_whole, down_turned = (
        lax.all_gather(value_weight, "fs", axis=0, tiled=True),
        lax.all_gather(gate_weight, "fs", axis=0, tiled=True),
        lax.all_gather(out_turned_shard, "fs", axis=0, tiled=True),
        lax.all_gather(up_weight, "fs", axis=0, tiled=True),
        lax.all_gather(down_turned_shard, "fs", axis=0, tiled=True),
    )
    normed = norm_rows(
        stream.reshape(token_count, model_width).astype(jnp.float32), in_gain
    ).astype(jnp.bfloat16)
    channels = value_weight.shape[1]
    values = jnp.dot(normed, value_whole, preferred_element_type=jnp.float32)
    gating = jnp.dot(normed, gate_whole, preferred_element_type=jnp.float32)
    gated = (values * jax.nn.sigmoid(gating)).astype(jnp.bfloat16)
    convolved = lax.conv_general_dilated(
        gated.reshape(seq_count, seq_length, channels),
        conv_kernel[:, None, :],
        window_strides=(1,),
        padding=[(KW - 1, 0)],
        dimension_numbers=("NWC", "WIO", "NWC"),
        feature_group_count=channels,
        preferred_element_type=jnp.float32,
    ).reshape(token_count, channels)
    conv_sums = lax.psum(row_sums(convolved), "tp")
    activated = jax.nn.silu(
        norm_shares(convolved, conv_sums, channels * tp_count, conv_gain) + conv_shift
    ).astype(jnp.bfloat16)
    partial_terms = contract(activated, out_turned)
    mixed = lax.psum_scatter(
        partial_terms.astype(jnp.bfloat16), "tp", scatter_dimension=1, tiled=True
    )
    normed_own = lax.dynamic_slice_in_dim(normed, tp_index * slice_width, slice_width, 1)
    gain_own = lax.dynamic_slice_in_dim(norm_gain, tp_index * slice_width, slice_width, 0)
    summed = residual_scale * normed_own.astype(jnp.float32) + mixed.astype(jnp.float32)
    mix_sums = lax.psum(row_sums(summed), "tp")
    settled_own = norm_shares(summed, mix_sums, model_width, gain_own).astype(jnp.bfloat16)
    settled_full = lax.all_gather(settled_own, "tp", axis=1, tiled=True)
    hidden = jnp.square(
        jax.nn.relu(jnp.dot(settled_full, up_whole, preferred_element_type=jnp.float32))
    ).astype(jnp.bfloat16)
    fed_terms = contract(hidden, down_turned)
    fed = lax.psum_scatter(fed_terms.astype(jnp.bfloat16), "tp", scatter_dimension=1, tiled=True)
    final_sum = residual_scale * settled_own.astype(jnp.float32) + fed.astype(jnp.float32)
    out_sums = lax.psum(row_sums(final_sum), "tp")
    result = norm_shares(final_sum, out_sums, model_width, out_gain).astype(jnp.bfloat16)
    return result.reshape(seq_count, seq_length, slice_width)


def to_rows(sums, squares):
    lane = lax.broadcasted_iota(jnp.int32, (sums.shape[0], 128), 1)
    spread = jnp.where(lane == 0, sums, jnp.where(lane == 1, squares, 0.0))
    return jnp.transpose(spread)[:8]


def from_rows(rows):
    filler = jnp.zeros((128 - rows.shape[0], rows.shape[1]), jnp.float32)
    columns = jnp.transpose(jnp.concatenate([rows, filler], axis=0))
    return columns[:, 0:1], columns[:, 1:2]


def normalize(values, sums, squares, width, gain):
    mean = sums / width
    var = squares / width - mean * mean
    return (values - mean) * lax.rsqrt(var + norm_epsilon) * gain


def layer_kernel(
    fs_count,
    seq_length,
    stream,
    in_gain,
    value_weight,
    gate_weight,
    conv_kernel,
    conv_gain,
    conv_shift,
    out_weight,
    norm_gain,
    up_hbm,
    down_hbm,
    out_gain,
    out,
    up,
    down,
    normed_send,
    normed_all,
    gate_send,
    gate_recv,
    padded,
    stat_send,
    stat_recv,
    active_all,
    mix_send,
    mix_recv,
    settled_all,
    settled_turned,
    up_send,
    up_recv,
    hidden_all,
    fed_total,
    fed_send,
    fed_recv,
    load_sem,
    normed_ss,
    normed_rs,
    gate_ss,
    gate_rs,
    stat_ss,
    stat_rs,
    active_ss,
    active_rs,
    mix_ss,
    mix_rs,
    settled_ss,
    settled_rs,
    turned_ss,
    turned_rs,
    up_ss,
    up_rs,
    hidden_ss,
    hidden_rs,
    fed_ss,
    fed_rs,
):
    n = fs_count
    f = lax.axis_index("fs")
    t = lax.axis_index("tp")
    rows, width = stream.shape
    own_width = width // n
    channels = value_weight.shape[1]
    chunks, _, chunk = up_send.shape[1:]
    bf16, f32 = jnp.bfloat16, jnp.float32

    def remote(src, dst, ss, rs, fs, tp):
        return pltpu.make_async_remote_copy(
            src_ref=src,
            dst_ref=dst,
            send_sem=ss,
            recv_sem=rs,
            device_id={"fs": fs, "tp": tp},
            device_id_type=pl.DeviceIdType.MESH,
        )

    def dot(left, right):
        return jnp.dot(left, right, preferred_element_type=f32)

    up_load = pltpu.make_async_copy(up_hbm, up, load_sem.at[0])
    down_load = pltpu.make_async_copy(down_hbm, down, load_sem.at[1])
    up_load.start()
    down_load.start()
    barrier = pltpu.get_barrier_semaphore()
    for a in range(n):
        for b in range(n):
            if a or b:
                pl.semaphore_signal(
                    barrier,
                    inc=1,
                    device_id={"fs": lax.rem(f + a, n), "tp": lax.rem(t + b, n)},
                    device_id_type=pl.DeviceIdType.MESH,
                )

    def norm_in(i, carry):
        at = pl.ds(pl.multiple_of(i * 16, 16), 16)
        normed = norm_rows(stream[at, :].astype(f32), in_gain[...]).astype(bf16)
        for a in range(n):
            normed_send[a, at, :] = normed[:, a * own_width : (a + 1) * own_width]
        return carry

    lax.fori_loop(0, rows // 16, norm_in, 0)
    pl.semaphore_wait(barrier, n * n - 1)

    def peer(base, j):
        return lax.rem(base + j, n)

    waits = []
    for j in range(1, n):
        to = peer(f, j)
        copy = remote(normed_send.at[to], normed_all.at[f], normed_ss.at[to], normed_rs.at[f], to, t)
        copy.start()
        waits.append(copy)
    normed_all[f] = normed_send[f]

    for j in range(1, n + 1):
        to = peer(f, j)
        if j < n:
            remote(normed_send.at[to], normed_all.at[to], normed_ss.at[to], normed_rs.at[to], to, t).wait_recv()
        values = dot(normed_all[to], value_weight[...])
        gating = dot(normed_all[to], gate_weight[...])
        if j < n:
            gate_send[to, :, :channels] = values.astype(bf16)
            gate_send[to, :, channels:] = gating.astype(bf16)
            copy = remote(gate_send.at[to], gate_recv.at[f], gate_ss.at[to], gate_rs.at[f], to, t)
            copy.start()
            waits.append(copy)
    for j in range(1, n):
        at = peer(f, j)
        remote(gate_send.at[at], gate_recv.at[at], gate_ss.at[at], gate_rs.at[at], at, t).wait_recv()
        got = gate_recv[at].astype(f32)
        values = values + got[:, :channels]
        gating = gating + got[:, channels:]
    gated = (values * jax.nn.sigmoid(gating)).astype(bf16).astype(f32)

    taps = conv_kernel.shape[0]
    pad = padded.shape[1] - seq_length
    pieces = []
    for s in range(rows // seq_length):
        padded[s, :pad, :] = jnp.zeros((pad, channels), f32)
        padded[s, pad:, :] = gated[s * seq_length : (s + 1) * seq_length]
        total = jnp.zeros((seq_length, channels), f32)
        for k in range(taps):
            start = pad - (taps - 1) + k
            total = total + padded[s, start : start + seq_length, :] * conv_kernel[k : k + 1, :].astype(f32)
        pieces.append(total)
    convolved = pieces[0] if len(pieces) == 1 else jnp.concatenate(pieces, axis=0)

    def shared_sums(which, values, axis):
        sums = jnp.sum(values, axis=1, keepdims=True)
        squares = jnp.sum(values * values, axis=1, keepdims=True)
        mine = to_rows(sums, squares)
        stat_send[which] = mine
        me = f if axis == "fs" else t
        for j in range(1, n):
            to = peer(me, j)
            copy = remote(
                stat_send.at[which],
                stat_recv.at[which, me],
                stat_ss.at[which, to],
                stat_rs.at[which, me],
                to if axis == "fs" else f,
                to if axis == "tp" else t,
            )
            copy.start()
            waits.append(copy)
        for j in range(1, n):
            at = peer(me, j)
            remote(
                stat_send.at[which],
                stat_recv.at[which, at],
                stat_ss.at[which, at],
                stat_rs.at[which, at],
                at if axis == "fs" else f,
                at if axis == "tp" else t,
            ).wait_recv()
            mine = mine + stat_recv[which, at]
        return from_rows(mine)

    sums, squares = shared_sums(0, convolved, "tp")
    activated = jax.nn.silu(
        normalize(convolved, sums, squares, channels * n, conv_gain[...]) + conv_shift[...]
    ).astype(bf16)
    active_all[f] = activated
    for j in range(1, n):
        to = peer(f, j)
        copy = remote(active_all.at[f], active_all.at[f], active_ss.at[to], active_rs.at[f], to, t)
        copy.start()
        waits.append(copy)

    for j in range(1, n + 1):
        at = peer(t, j)

        @pl.when(at != f)
        def _():
            remote(active_all.at[at], active_all.at[at], active_ss.at[at], active_rs.at[at], at, t).wait_recv()

        mix_send[at] = dot(active_all[at], out_weight[...]).astype(bf16)
        if j < n:
            copy = remote(mix_send.at[at], mix_recv.at[t], mix_ss.at[at], mix_rs.at[t], f, at)
            copy.start()
            waits.append(copy)
    mixed = mix_send[t].astype(f32)
    for j in range(1, n):
        at = peer(t, j)
        remote(mix_send.at[at], mix_recv.at[at], mix_ss.at[at], mix_rs.at[at], f, at).wait_recv()
        mixed = mixed + mix_recv[at].astype(f32)
    summed = residual_scale * normed_all[t].astype(f32) + mixed.astype(bf16).astype(f32)
    sums, squares = shared_sums(1, summed, "fs")
    gain_own = norm_gain[:, pl.ds(pl.multiple_of(f * own_width, 128), own_width)]
    settled_all[t] = normalize(summed, sums, squares, width, gain_own).astype(bf16)
    for j in range(1, n):
        to = peer(t, j)
        copy = remote(settled_all.at[t], settled_all.at[t], settled_ss.at[to], settled_rs.at[t], f, to)
        copy.start()
        waits.append(copy)
    turned = remote(settled_all.at[t], settled_turned, turned_ss, turned_rs, t, f)

    @pl.when(f != t)
    def _():
        turned.start()

    @pl.when(f == t)
    def _():
        settled_turned[...] = settled_all[t]

    up_load.wait()
    for j in range(1, n):
        at = peer(t, j)
        remote(settled_all.at[at], settled_all.at[at], settled_ss.at[at], settled_rs.at[at], f, at).wait_recv()

    def columns(c):
        return pl.ds(pl.multiple_of(c * chunk, 128), chunk)

    def up_step(c, carry):
        for j in range(1, n):
            to = peer(f, j)
            up_send[to, c] = dot(settled_all[to], up[:, columns(c)]).astype(bf16)
            remote(up_send.at[to, c], up_recv.at[f, c], up_ss.at[to, c], up_rs.at[f, c], to, t).start()
        return carry

    lax.fori_loop(0, chunks, up_step, 0)

    def hidden_step(c, carry):
        total = dot(settled_all[f], up[:, columns(c)])
        for j in range(1, n):
            at = peer(f, j)
            remote(up_send.at[at, c], up_recv.at[at, c], up_ss.at[at, c], up_rs.at[at, c], at, t).wait()
            total = total + up_recv[at, c].astype(f32)
        hidden_all[f, c] = jnp.square(jnp.maximum(total, 0.0)).astype(bf16)
        for j in range(1, n):
            to = peer(f, j)
            remote(
                hidden_all.at[f, c], hidden_all.at[f, c], hidden_ss.at[to, c], hidden_rs.at[f, c], to, t
            ).start()
        return carry

    lax.fori_loop(0, chunks, hidden_step, 0)
    down_load.wait()
    fed_total[...] = jnp.zeros_like(fed_total)

    def down_step(c, carry):
        part = down[pl.ds(pl.multiple_of(c * chunk, 128), chunk), :]
        for j in range(n):
            at = peer(f, j)
            if j > 0:
                remote(
                    hidden_all.at[at, c], hidden_all.at[at, c], hidden_ss.at[at, c], hidden_rs.at[at, c], at, t
                ).wait()
            fed_total[at] += dot(hidden_all[at, c], part)
        return carry

    lax.fori_loop(0, chunks, down_step, 0)
    for j in range(1, n + 1):
        at = peer(f, j)
        fed_send[at] = fed_total[at].astype(bf16)
        copy = remote(fed_send.at[at], fed_recv.at[t], fed_ss.at[at], fed_rs.at[t], at, f)
        if j < n:
            copy.start()
            waits.append(copy)
        else:

            @pl.when(f != t)
            def _():
                copy.start()

            @pl.when(f == t)
            def _():
                fed_recv[t] = fed_send[f]

    last = copy

    @pl.when(f != t)
    def _():
        turned.wait()

    fed = jnp.zeros((rows, own_width), f32)
    for b in range(n):
        got = remote(fed_send.at[b], fed_recv.at[b], fed_ss.at[b], fed_rs.at[b], t, b)

        @pl.when(jnp.logical_not(jnp.logical_and(f == t, t == b)))
        def _():
            got.wait_recv()

        fed = fed + fed_recv[b].astype(f32)
    final = residual_scale * settled_turned[...].astype(f32) + fed.astype(bf16).astype(f32)
    sums, squares = shared_sums(2, final, "tp")
    out[...] = normalize(final, sums, squares, width, out_gain[...]).astype(bf16)
    for copy in waits:
        copy.wait_send()

    @pl.when(f != t)
    def _():
        last.wait_send()


def fast_shards(
    stream,
    in_gain,
    value_weight,
    gate_weight,
    conv_kernel,
    conv_gain,
    conv_shift,
    out_weight,
    norm_gain,
    up_weight,
    down_weight,
    out_gain,
):
    seq_count, seq_length, width = stream.shape
    rows = seq_count * seq_length
    n = lax.axis_size("fs")
    own = width // n
    channels = value_weight.shape[1]
    units = up_weight.shape[1]
    chunk = units // 4
    chunks = units // chunk
    taps = conv_kernel.shape[0]
    pad = -(-(taps - 1) // 8) * 8
    bf16, f32 = jnp.bfloat16, jnp.float32
    vmem, dma = pltpu.VMEM, pltpu.SemaphoreType.DMA
    whole = pl.BlockSpec(memory_space=pltpu.VMEM)
    far = pl.BlockSpec(memory_space=pl.ANY)
    result = pl.pallas_call(
        functools.partial(layer_kernel, n, seq_length),
        out_shape=jax.ShapeDtypeStruct((rows, own), bf16),
        in_specs=[whole] * 9 + [far, far, whole],
        out_specs=whole,
        scratch_shapes=[
            vmem(up_weight.shape, bf16),
            vmem(down_weight.shape, bf16),
            vmem((n, rows, own), bf16),
            vmem((n, rows, own), bf16),
            vmem((n, rows, 2 * channels), bf16),
            vmem((n, rows, 2 * channels), bf16),
            vmem((seq_count, pad + seq_length, channels), f32),
            vmem((3, 8, rows), f32),
            vmem((3, n, 8, rows), f32),
            vmem((n, rows, channels), bf16),
            vmem((n, rows, own), bf16),
            vmem((n, rows, own), bf16),
            vmem((n, rows, own), bf16),
            vmem((rows, own), bf16),
            vmem((n, chunks, rows, chunk), bf16),
            vmem((n, chunks, rows, chunk), bf16),
            vmem((n, chunks, rows, chunk), bf16),
            vmem((n, rows, own), f32),
            vmem((n, rows, own), bf16),
            vmem((n, rows, own), bf16),
            dma((2,)),
            dma((n,)),
            dma((n,)),
            dma((n,)),
            dma((n,)),
            dma((3, n)),
            dma((3, n)),
            dma((n,)),
            dma((n,)),
            dma((n,)),
            dma((n,)),
            dma((n,)),
            dma((n,)),
            dma,
            dma,
            dma((n, chunks)),
            dma((n, chunks)),
            dma((n, chunks)),
            dma((n, chunks)),
            dma((n,)),
            dma((n,)),
        ],
        compiler_params=pltpu.CompilerParams(
            collective_id=0, has_side_effects=True, vmem_limit_bytes=60 * 1024 * 1024
        ),
    )(
        stream.reshape(rows, width),
        in_gain[None],
        value_weight,
        gate_weight,
        conv_kernel,
        conv_gain[None],
        conv_shift[None],
        out_weight,
        norm_gain[None],
        up_weight,
        down_weight,
        out_gain[None],
    )
    return result.reshape(seq_count, seq_length, own)


def layer(*args):
    stream, value_weight, up_weight = args[0], args[2], args[9]
    n = lax.axis_size("fs")
    fits = (
        n == lax.axis_size("tp")
        and n > 1
        and stream.shape[0] * stream.shape[1] == 128
        and stream.shape[1] % 8 == 0
        and stream.shape[2] % (128 * n) == 0
        and value_weight.shape[1] % 128 == 0
        and up_weight.shape[1] % 512 == 0
    )
    return fast_shards(*args) if fits else shards(*args)


def solution(mesh):
    in_specs = (
        P(("grp", "fs"), None, None),
        P(),
        P("fs", "tp"),
        P("fs", "tp"),
        P(None, "tp"),
        P("tp"),
        P("tp"),
        P("tp", "fs"),
        P(),
        P("fs", "tp"),
        P("tp", "fs"),
        P("tp"),
    )
    out_specs = P(("grp", "fs"), None, "tp")
    return jax.shard_map(layer, mesh=mesh, in_specs=in_specs, out_specs=out_specs, check_vma=False)
```

```python
import functools

import jax
import jax.numpy as jnp
from jax import lax
from jax.experimental import pallas as pl
from jax.experimental.pallas import tpu as pltpu
from jax.sharding import PartitionSpec as P

KW = 31
UP_A, UP_B, DN_A, DN_B = (1, 2), (3,), (1, 2), (3,)


norm_epsilon = 1e-05
residual_scale = 2.0**0.25


def norm_rows(values, gain_vector):
    row_mean = jnp.mean(values, axis=-1, keepdims=True)
    row_var = jnp.mean(jnp.square(values - row_mean), axis=-1, keepdims=True)
    return (values - row_mean) * lax.rsqrt(row_var + norm_epsilon) * gain_vector


def norm_shares(summed, stat_sums, full_width, gain_vector):
    row_mean = stat_sums[0] / full_width
    row_var = stat_sums[1] / full_width - row_mean * row_mean
    return (summed - row_mean[:, None]) * lax.rsqrt(row_var + norm_epsilon)[:, None] * gain_vector


def row_sums(summed):
    return (jnp.sum(summed, axis=1), jnp.sum(summed * summed, axis=1))


def contract(left, turned):
    return lax.dot_general(
        left, turned, (((1,), (1,)), ((), ())), preferred_element_type=jnp.float32
    )


def shards(
    stream,
    in_gain,
    value_weight,
    gate_weight,
    conv_kernel,
    conv_gain,
    conv_shift,
    out_weight,
    norm_gain,
    up_weight,
    down_weight,
    out_gain,
):
    seq_count, seq_length, model_width = stream.shape
    token_count = seq_count * seq_length
    tp_count = lax.axis_size("tp")
    slice_width = model_width // tp_count
    tp_index = lax.axis_index("tp")
    out_turned_shard = out_weight.T
    down_turned_shard = down_weight.T
    value_whole, gate_whole, out_turned, up_whole, down_turned = (
        lax.all_gather(value_weight, "fs", axis=0, tiled=True),
        lax.all_gather(gate_weight, "fs", axis=0, tiled=True),
        lax.all_gather(out_turned_shard, "fs", axis=0, tiled=True),
        lax.all_gather(up_weight, "fs", axis=0, tiled=True),
        lax.all_gather(down_turned_shard, "fs", axis=0, tiled=True),
    )
    normed = norm_rows(
        stream.reshape(token_count, model_width).astype(jnp.float32), in_gain
    ).astype(jnp.bfloat16)
    channels = value_weight.shape[1]
    values = jnp.dot(normed, value_whole, preferred_element_type=jnp.float32)
    gating = jnp.dot(normed, gate_whole, preferred_element_type=jnp.float32)
    gated = (values * jax.nn.sigmoid(gating)).astype(jnp.bfloat16)
    convolved = lax.conv_general_dilated(
        gated.reshape(seq_count, seq_length, channels),
        conv_kernel[:, None, :],
        window_strides=(1,),
        padding=[(KW - 1, 0)],
        dimension_numbers=("NWC", "WIO", "NWC"),
        feature_group_count=channels,
        preferred_element_type=jnp.float32,
    ).reshape(token_count, channels)
    conv_sums = lax.psum(row_sums(convolved), "tp")
    activated = jax.nn.silu(
        norm_shares(convolved, conv_sums, channels * tp_count, conv_gain) + conv_shift
    ).astype(jnp.bfloat16)
    partial_terms = contract(activated, out_turned)
    mixed = lax.psum_scatter(
        partial_terms.astype(jnp.bfloat16), "tp", scatter_dimension=1, tiled=True
    )
    normed_own = lax.dynamic_slice_in_dim(normed, tp_index * slice_width, slice_width, 1)
    gain_own = lax.dynamic_slice_in_dim(norm_gain, tp_index * slice_width, slice_width, 0)
    summed = residual_scale * normed_own.astype(jnp.float32) + mixed.astype(jnp.float32)
    mix_sums = lax.psum(row_sums(summed), "tp")
    settled_own = norm_shares(summed, mix_sums, model_width, gain_own).astype(jnp.bfloat16)
    settled_full = lax.all_gather(settled_own, "tp", axis=1, tiled=True)
    hidden = jnp.square(
        jax.nn.relu(jnp.dot(settled_full, up_whole, preferred_element_type=jnp.float32))
    ).astype(jnp.bfloat16)
    fed_terms = contract(hidden, down_turned)
    fed = lax.psum_scatter(fed_terms.astype(jnp.bfloat16), "tp", scatter_dimension=1, tiled=True)
    final_sum = residual_scale * settled_own.astype(jnp.float32) + fed.astype(jnp.float32)
    out_sums = lax.psum(row_sums(final_sum), "tp")
    result = norm_shares(final_sum, out_sums, model_width, out_gain).astype(jnp.bfloat16)
    return result.reshape(seq_count, seq_length, slice_width)


def to_rows(sums, squares):
    lane = lax.broadcasted_iota(jnp.int32, (sums.shape[0], 128), 1)
    spread = jnp.where(lane == 0, sums, jnp.where(lane == 1, squares, 0.0))
    return jnp.transpose(spread)[:8]


def from_rows(rows):
    filler = jnp.zeros((128 - rows.shape[0], rows.shape[1]), jnp.float32)
    columns = jnp.transpose(jnp.concatenate([rows, filler], axis=0))
    return columns[:, 0:1], columns[:, 1:2]


def normalize(values, sums, squares, width, gain):
    mean = sums / width
    var = squares / width - mean * mean
    return (values - mean) * lax.rsqrt(var + norm_epsilon) * gain


def layer_kernel(
    fs_count,
    seq_length,
    stream,
    in_gain,
    value_weight,
    gate_weight,
    conv_kernel,
    conv_gain,
    conv_shift,
    out_weight,
    norm_gain,
    up_hbm,
    down_hbm,
    out_gain,
    out,
    up,
    down,
    normed_send,
    normed_all,
    gate_send,
    gate_recv,
    padded,
    stat_send,
    stat_recv,
    active_all,
    mix_send,
    mix_recv,
    settled_all,
    hidden,
    pair_own,
    pair_send,
    pair_recv,
    cross_send,
    cross_recv,
    fed_send,
    fed_recv,
    load_sem,
    up_ss,
    up_rs,
    down_ss,
    down_rs,
    normed_ss,
    normed_rs,
    gate_ss,
    gate_rs,
    stat_ss,
    stat_rs,
    active_ss,
    active_rs,
    mix_ss,
    mix_rs,
    settled_ss,
    settled_rs,
    pair_ss,
    pair_rs,
    cross_ss,
    cross_rs,
    fed_ss,
    fed_rs,
):
    n = fs_count
    f = lax.axis_index("fs")
    t = lax.axis_index("tp")
    g = lax.axis_index("grp")
    side = lax.rem(t, 2)
    mate = t + 1 - 2 * side
    across = lax.rem(t + 2, n)
    rows, width = stream.shape
    own_width = width // n
    channels = value_weight.shape[1]
    half_units = up.shape[3]
    units = 2 * half_units
    bf16, f32 = jnp.bfloat16, jnp.float32

    def remote(src, dst, ss, rs, fs, tp, grp=g):
        return pltpu.make_async_remote_copy(
            src_ref=src,
            dst_ref=dst,
            send_sem=ss,
            recv_sem=rs,
            device_id={"grp": grp, "fs": fs, "tp": tp},
            device_id_type=pl.DeviceIdType.MESH,
        )

    def dot(left, right):
        return jnp.dot(left, right, preferred_element_type=f32)

    def share(block, h):
        return pl.ds(pl.multiple_of(block * units + h * half_units, 128), half_units)

    loads = []
    for h in range(2):
        loads.append(pltpu.make_async_copy(up_hbm.at[:, share(f, h)], up.at[h, f], load_sem.at[0, h]))
        loads.append(pltpu.make_async_copy(down_hbm.at[share(f, h), :], down.at[h, f], load_sem.at[1, h]))
    for load in loads:
        load.start()
    barrier = pltpu.get_barrier_semaphore()
    for a in range(n):
        for b in range(n):
            if a or b:
                pl.semaphore_signal(
                    barrier,
                    inc=1,
                    device_id={"fs": lax.rem(f + a, n), "tp": lax.rem(t + b, n)},
                    device_id_type=pl.DeviceIdType.MESH,
                )

    pl.semaphore_signal(
        barrier,
        inc=1,
        device_id={"grp": 1 - g, "fs": f, "tp": t},
        device_id_type=pl.DeviceIdType.MESH,
    )

    def norm_in(i, carry):
        at = pl.ds(pl.multiple_of(i * 16, 16), 16)
        normed = norm_rows(stream[at, :].astype(f32), in_gain[...]).astype(bf16)
        for a in range(n):
            normed_send[a, at, :] = normed[:, a * own_width : (a + 1) * own_width]
        return carry

    lax.fori_loop(0, rows // 16, norm_in, 0)
    def peer(base, j):
        return lax.rem(base + j, n)

    waits = []

    def up_copy(to, at):
        return remote(up_hbm.at[:, share(to, g)], up.at[g, at], up_ss.at[0, to], up_rs.at[0, at], to, t)

    def down_copy(to, at):
        return remote(down_hbm.at[share(to, g), :], down.at[g, at], down_ss.at[0, to], down_rs.at[0, at], to, t)

    def start(copy):
        copy.start()
        waits.append(copy)

    def send_weights(make, steps):
        for j in steps:
            start(make(peer(f, j), f))

    def swap_weights(make, held, ss, rs):
        for j in range(1, n):
            at = peer(f, n - j)
            make(at, at).wait_recv()
            start(remote(held.at[g, at], held.at[g, at], ss.at[1, at], rs.at[1, at], f, t, 1 - g))

    def swap_wait(held, ss, rs):
        for j in range(1, n):
            at = peer(f, n - j)
            remote(held.at[1 - g, at], held.at[1 - g, at], ss.at[1, at], rs.at[1, at], f, t, 1 - g).wait_recv()

    half = rows // 2
    mine = pl.ds(pl.multiple_of(side * half, half), half)
    theirs = pl.ds(pl.multiple_of((1 - side) * half, half), half)

    def normed_copy(to, at):
        return remote(
            normed_send.at[to, mine], normed_all.at[at, mine], normed_ss.at[0, to], normed_rs.at[0, at], to, t
        )

    def normed_pass(at, part):
        return remote(
            normed_all.at[at, part], normed_all.at[at, part], normed_ss.at[1, at], normed_rs.at[1, at], f, mate
        )

    pl.semaphore_wait(barrier, n * n)
    for j in range(1, n):
        start(normed_copy(peer(f, j), f))
    send_weights(up_copy, UP_A)
    normed_all[f] = normed_send[f]
    for j in range(1, n):
        at = peer(f, j)
        normed_copy(at, at).wait_recv()
        start(normed_pass(at, mine))

    for j in range(1, n + 1):
        to = peer(f, j)
        if j < n:
            normed_pass(to, theirs).wait_recv()
        values = dot(normed_all[to], value_weight[...])
        gating = dot(normed_all[to], gate_weight[...])
        if j < n:
            gate_send[to, :, :channels] = values.astype(bf16)
            gate_send[to, :, channels:] = gating.astype(bf16)
            copy = remote(gate_send.at[to], gate_recv.at[f], gate_ss.at[to], gate_rs.at[f], to, t)
            copy.start()
            waits.append(copy)
    send_weights(up_copy, UP_B)
    for j in range(1, n):
        at = peer(f, j)
        remote(gate_send.at[at], gate_recv.at[at], gate_ss.at[at], gate_rs.at[at], at, t).wait_recv()
        got = gate_recv[at].astype(f32)
        values = values + got[:, :channels]
        gating = gating + got[:, channels:]
    gated = (values * jax.nn.sigmoid(gating)).astype(bf16).astype(f32)

    taps = conv_kernel.shape[0]
    pad = padded.shape[1] - seq_length
    pieces = []
    for s in range(rows // seq_length):
        padded[s, :pad, :] = jnp.zeros((pad, channels), f32)
        padded[s, pad:, :] = gated[s * seq_length : (s + 1) * seq_length]
        total = jnp.zeros((seq_length, channels), f32)
        for k in range(taps):
            begin = pad - (taps - 1) + k
            total = total + padded[s, begin : begin + seq_length, :] * conv_kernel[k : k + 1, :].astype(f32)
        pieces.append(total)
    convolved = pieces[0] if len(pieces) == 1 else jnp.concatenate(pieces, axis=0)

    def shared_sums(which, values, axis, then=()):
        sums = jnp.sum(values, axis=1, keepdims=True)
        squares = jnp.sum(values * values, axis=1, keepdims=True)
        mine = to_rows(sums, squares)
        stat_send[which] = mine
        me = f if axis == "fs" else t
        for j in range(1, n):
            to = peer(me, j)
            copy = remote(
                stat_send.at[which],
                stat_recv.at[which, me],
                stat_ss.at[which, to],
                stat_rs.at[which, me],
                to if axis == "fs" else f,
                to if axis == "tp" else t,
            )
            copy.start()
            waits.append(copy)
        send_weights(down_copy, then)
        for j in range(1, n):
            at = peer(me, j)
            remote(
                stat_send.at[which],
                stat_recv.at[which, at],
                stat_ss.at[which, at],
                stat_rs.at[which, at],
                at if axis == "fs" else f,
                at if axis == "tp" else t,
            ).wait_recv()
            mine = mine + stat_recv[which, at]
        return from_rows(mine)

    sums, squares = shared_sums(0, convolved, "tp")
    activated = jax.nn.silu(
        normalize(convolved, sums, squares, channels * n, conv_gain[...]) + conv_shift[...]
    ).astype(bf16)
    active_all[f] = activated
    for j in range(1, n):
        to = peer(f, j)
        start(remote(active_all.at[f], active_all.at[f], active_ss.at[to], active_rs.at[f], to, t))
    send_weights(down_copy, DN_A)
    swap_weights(up_copy, up, up_ss, up_rs)

    for j in range(1, n + 1):
        at = peer(t, j)

        @pl.when(at != f)
        def _():
            remote(active_all.at[at], active_all.at[at], active_ss.at[at], active_rs.at[at], at, t).wait_recv()

        mix_send[at] = dot(active_all[at], out_weight[...]).astype(bf16)
        if j < n:
            copy = remote(mix_send.at[at], mix_recv.at[t], mix_ss.at[at], mix_rs.at[t], f, at)
            copy.start()
            waits.append(copy)
    mixed = mix_send[t].astype(f32)
    for j in range(1, n):
        at = peer(t, j)
        remote(mix_send.at[at], mix_recv.at[at], mix_ss.at[at], mix_rs.at[at], f, at).wait_recv()
        mixed = mixed + mix_recv[at].astype(f32)
    summed = residual_scale * normed_all[t].astype(f32) + mixed.astype(bf16).astype(f32)
    sums, squares = shared_sums(1, summed, "fs", DN_B)
    gain_own = norm_gain[:, pl.ds(pl.multiple_of(f * own_width, 128), own_width)]
    settled_all[t, f] = normalize(summed, sums, squares, width, gain_own).astype(bf16)

    def settled_copy(step, group, block, fs, tp, key=None):
        where = settled_all.at[group, block]
        send = block if key is None else key
        return remote(where, where, settled_ss.at[step, send], settled_rs.at[step, block], fs, tp)

    for j in range(1, n):
        start(settled_copy(0, t, f, peer(f, j), t, peer(f, j)))
    for j in range(n):
        at = peer(f, j)
        if j > 0:
            settled_copy(0, t, at, at, t).wait_recv()
        start(settled_copy(1, t, at, f, across))
        start(settled_copy(2, t, at, f, mate))
    for j in range(n):
        at = peer(f, j)
        settled_copy(1, across, at, f, across).wait_recv()
        start(settled_copy(3, across, at, f, mate))
    swap_weights(down_copy, down, down_ss, down_rs)
    for load in loads:
        load.wait()
    swap_wait(up, up_ss, up_rs)

    def make_hidden(group):
        for h in range(2):
            total = jnp.zeros((rows, half_units), f32)
            for b in range(n):
                total = total + dot(settled_all[group, b], up[h, b])
            hidden[group, h] = jnp.square(jnp.maximum(total, 0.0)).astype(bf16)

    make_hidden(t)
    for j in range(n):
        at = peer(f, j)
        settled_copy(2, mate, at, f, mate).wait_recv()
    make_hidden(mate)
    make_hidden(across)
    opposite = lax.rem(mate + 2, n)
    for j in range(n):
        at = peer(f, j)
        settled_copy(3, opposite, at, f, mate).wait_recv()
    make_hidden(opposite)
    swap_wait(down, down_ss, down_rs)

    def fed_part(group, block):
        return dot(hidden[group, 0], down[0, block]) + dot(hidden[group, 1], down[1, block])

    def pair_copy(r):
        return remote(pair_send.at[r], pair_recv.at[r], pair_ss.at[r], pair_rs.at[r], f, mate)

    def cross_copy(r):
        return remote(cross_send.at[r], cross_recv.at[r], cross_ss.at[r], cross_rs.at[r], f, across)

    for j in range(1, n + 1):
        r = peer(f, j)
        pair_send[r, 0] = fed_part(r, mate).astype(bf16)
        pair_send[r, 1] = fed_part(r, opposite).astype(bf16)
        start(pair_copy(r))
        pair_own[r, 0] = fed_part(r, t)
        pair_own[r, 1] = fed_part(r, across)
        pair_copy(r).wait_recv()
        pair_own[r, 0] += pair_recv[r, 0].astype(f32)
        cross_send[r] = (pair_own[r, 1] + pair_recv[r, 1].astype(f32)).astype(bf16)
        start(cross_copy(r))
    for j in range(1, n + 1):
        r = peer(f, j)
        cross_copy(r).wait_recv()
        fed = pair_own[r, 0] + cross_recv[r].astype(f32)
        if j < n:
            fed_send[r] = fed.astype(bf16)
            start(remote(fed_send.at[r], fed_recv.at[f], fed_ss.at[r], fed_rs.at[f], r, t))
    for j in range(1, n):
        at = peer(f, j)
        remote(fed_send.at[at], fed_recv.at[at], fed_ss.at[at], fed_rs.at[at], at, t).wait_recv()
        fed = fed + fed_recv[at].astype(f32)
    final = residual_scale * settled_all[f, t].astype(f32) + fed.astype(bf16).astype(f32)
    sums, squares = shared_sums(2, final, "tp")
    out[...] = normalize(final, sums, squares, width, out_gain[...]).astype(bf16)
    for copy in waits:
        copy.wait_send()


def fast_shards(
    stream,
    in_gain,
    value_weight,
    gate_weight,
    conv_kernel,
    conv_gain,
    conv_shift,
    out_weight,
    norm_gain,
    up_weight,
    down_weight,
    out_gain,
):
    seq_count, seq_length, width = stream.shape
    rows = seq_count * seq_length
    n = lax.axis_size("fs")
    own = width // n
    channels = value_weight.shape[1]
    units = up_weight.shape[1]
    half_units = units // n // 2
    taps = conv_kernel.shape[0]
    pad = -(-(taps - 1) // 8) * 8
    bf16, f32 = jnp.bfloat16, jnp.float32
    vmem, dma = pltpu.VMEM, pltpu.SemaphoreType.DMA
    whole = pl.BlockSpec(memory_space=pltpu.VMEM)
    far = pl.BlockSpec(memory_space=pl.ANY)
    result = pl.pallas_call(
        functools.partial(layer_kernel, n, seq_length),
        out_shape=jax.ShapeDtypeStruct((rows, own), bf16),
        in_specs=[whole] * 9 + [far, far, whole],
        out_specs=whole,
        scratch_shapes=[
            vmem((2, n, own, half_units), bf16),
            vmem((2, n, half_units, own), bf16),
            vmem((n, rows, own), bf16),
            vmem((n, rows, own), bf16),
            vmem((n, rows, 2 * channels), bf16),
            vmem((n, rows, 2 * channels), bf16),
            vmem((seq_count, pad + seq_length, channels), f32),
            vmem((3, 8, rows), f32),
            vmem((3, n, 8, rows), f32),
            vmem((n, rows, channels), bf16),
            vmem((n, rows, own), bf16),
            vmem((n, rows, own), bf16),
            vmem((n, n, rows, own), bf16),
            vmem((n, 2, rows, half_units), bf16),
            vmem((n, 2, rows, own), f32),
            vmem((n, 2, rows, own), bf16),
            vmem((n, 2, rows, own), bf16),
            vmem((n, rows, own), bf16),
            vmem((n, rows, own), bf16),
            vmem((n, rows, own), bf16),
            vmem((n, rows, own), bf16),
            dma((2, 2)),
            dma((2, n)),
            dma((2, n)),
            dma((2, n)),
            dma((2, n)),
            dma((2, n)),
            dma((2, n)),
            dma((n,)),
            dma((n,)),
            dma((3, n)),
            dma((3, n)),
            dma((n,)),
            dma((n,)),
            dma((n,)),
            dma((n,)),
            dma((4, n)),
            dma((4, n)),
            dma((n,)),
            dma((n,)),
            dma((n,)),
            dma((n,)),
            dma((n,)),
            dma((n,)),
        ],
        compiler_params=pltpu.CompilerParams(
            collective_id=0, has_side_effects=True, vmem_limit_bytes=60 * 1024 * 1024
        ),
    )(
        stream.reshape(rows, width),
        in_gain[None],
        value_weight,
        gate_weight,
        conv_kernel,
        conv_gain[None],
        conv_shift[None],
        out_weight,
        norm_gain[None],
        up_weight,
        down_weight,
        out_gain[None],
    )
    return result.reshape(seq_count, seq_length, own)


def layer(*args):
    stream, value_weight, up_weight = args[0], args[2], args[9]
    n = lax.axis_size("fs")
    fits = (
        n == lax.axis_size("tp")
        and n == 4
        and lax.axis_size("grp") == 2
        and stream.shape[0] * stream.shape[1] == 128
        and stream.shape[1] % 8 == 0
        and stream.shape[2] % (128 * n) == 0
        and value_weight.shape[1] % 128 == 0
        and up_weight.shape[1] % (256 * n) == 0
    )
    return fast_shards(*args) if fits else shards(*args)


def solution(mesh):
    in_specs = (
        P(("grp", "fs"), None, None),
        P(),
        P("fs", "tp"),
        P("fs", "tp"),
        P(None, "tp"),
        P("tp"),
        P("tp"),
        P("tp", "fs"),
        P(),
        P("fs", "tp"),
        P("tp", "fs"),
        P("tp"),
    )
    out_specs = P(("grp", "fs"), None, "tp")
    return jax.shard_map(layer, mesh=mesh, in_specs=in_specs, out_specs=out_specs, check_vma=False)
```

```python
import functools

import jax
import jax.numpy as jnp
from jax import lax
from jax.experimental import pallas as pl
from jax.experimental.pallas import tpu as pltpu
from jax.sharding import PartitionSpec as P

KW = 31
PLAN = ("u1u2u3", "d2", "", "U1U2U3", "d1d3", "D2", "", "D1D3", "", "", "")


norm_epsilon = 1e-05
residual_scale = 2.0**0.25


def norm_rows(values, gain_vector):
    row_mean = jnp.mean(values, axis=-1, keepdims=True)
    row_var = jnp.mean(jnp.square(values - row_mean), axis=-1, keepdims=True)
    return (values - row_mean) * lax.rsqrt(row_var + norm_epsilon) * gain_vector


def norm_shares(summed, stat_sums, full_width, gain_vector):
    row_mean = stat_sums[0] / full_width
    row_var = stat_sums[1] / full_width - row_mean * row_mean
    return (summed - row_mean[:, None]) * lax.rsqrt(row_var + norm_epsilon)[:, None] * gain_vector


def row_sums(summed):
    return (jnp.sum(summed, axis=1), jnp.sum(summed * summed, axis=1))


def contract(left, turned):
    return lax.dot_general(
        left, turned, (((1,), (1,)), ((), ())), preferred_element_type=jnp.float32
    )


def shards(
    stream,
    in_gain,
    value_weight,
    gate_weight,
    conv_kernel,
    conv_gain,
    conv_shift,
    out_weight,
    norm_gain,
    up_weight,
    down_weight,
    out_gain,
):
    seq_count, seq_length, model_width = stream.shape
    token_count = seq_count * seq_length
    tp_count = lax.axis_size("tp")
    slice_width = model_width // tp_count
    tp_index = lax.axis_index("tp")
    out_turned_shard = out_weight.T
    down_turned_shard = down_weight.T
    value_whole, gate_whole, out_turned, up_whole, down_turned = (
        lax.all_gather(value_weight, "fs", axis=0, tiled=True),
        lax.all_gather(gate_weight, "fs", axis=0, tiled=True),
        lax.all_gather(out_turned_shard, "fs", axis=0, tiled=True),
        lax.all_gather(up_weight, "fs", axis=0, tiled=True),
        lax.all_gather(down_turned_shard, "fs", axis=0, tiled=True),
    )
    normed = norm_rows(
        stream.reshape(token_count, model_width).astype(jnp.float32), in_gain
    ).astype(jnp.bfloat16)
    channels = value_weight.shape[1]
    values = jnp.dot(normed, value_whole, preferred_element_type=jnp.float32)
    gating = jnp.dot(normed, gate_whole, preferred_element_type=jnp.float32)
    gated = (values * jax.nn.sigmoid(gating)).astype(jnp.bfloat16)
    convolved = lax.conv_general_dilated(
        gated.reshape(seq_count, seq_length, channels),
        conv_kernel[:, None, :],
        window_strides=(1,),
        padding=[(KW - 1, 0)],
        dimension_numbers=("NWC", "WIO", "NWC"),
        feature_group_count=channels,
        preferred_element_type=jnp.float32,
    ).reshape(token_count, channels)
    conv_sums = lax.psum(row_sums(convolved), "tp")
    activated = jax.nn.silu(
        norm_shares(convolved, conv_sums, channels * tp_count, conv_gain) + conv_shift
    ).astype(jnp.bfloat16)
    partial_terms = contract(activated, out_turned)
    mixed = lax.psum_scatter(
        partial_terms.astype(jnp.bfloat16), "tp", scatter_dimension=1, tiled=True
    )
    normed_own = lax.dynamic_slice_in_dim(normed, tp_index * slice_width, slice_width, 1)
    gain_own = lax.dynamic_slice_in_dim(norm_gain, tp_index * slice_width, slice_width, 0)
    summed = residual_scale * normed_own.astype(jnp.float32) + mixed.astype(jnp.float32)
    mix_sums = lax.psum(row_sums(summed), "tp")
    settled_own = norm_shares(summed, mix_sums, model_width, gain_own).astype(jnp.bfloat16)
    settled_full = lax.all_gather(settled_own, "tp", axis=1, tiled=True)
    hidden = jnp.square(
        jax.nn.relu(jnp.dot(settled_full, up_whole, preferred_element_type=jnp.float32))
    ).astype(jnp.bfloat16)
    fed_terms = contract(hidden, down_turned)
    fed = lax.psum_scatter(fed_terms.astype(jnp.bfloat16), "tp", scatter_dimension=1, tiled=True)
    final_sum = residual_scale * settled_own.astype(jnp.float32) + fed.astype(jnp.float32)
    out_sums = lax.psum(row_sums(final_sum), "tp")
    result = norm_shares(final_sum, out_sums, model_width, out_gain).astype(jnp.bfloat16)
    return result.reshape(seq_count, seq_length, slice_width)


def to_rows(sums, squares):
    lane = lax.broadcasted_iota(jnp.int32, (sums.shape[0], 128), 1)
    spread = jnp.where(lane == 0, sums, jnp.where(lane == 1, squares, 0.0))
    return jnp.transpose(spread)[:8]


def from_rows(rows):
    filler = jnp.zeros((128 - rows.shape[0], rows.shape[1]), jnp.float32)
    columns = jnp.transpose(jnp.concatenate([rows, filler], axis=0))
    return columns[:, 0:1], columns[:, 1:2]


def normalize(values, sums, squares, width, gain):
    mean = sums / width
    var = squares / width - mean * mean
    return (values - mean) * lax.rsqrt(var + norm_epsilon) * gain


def layer_kernel(
    fs_count,
    seq_length,
    stream,
    in_gain,
    value_weight,
    gate_weight,
    conv_kernel,
    conv_gain,
    conv_shift,
    out_weight,
    norm_gain,
    up_hbm,
    down_hbm,
    out_gain,
    out,
    up,
    down,
    normed_send,
    normed_all,
    gate_send,
    gate_recv,
    padded,
    stat_send,
    stat_recv,
    active_all,
    mix_send,
    mix_recv,
    settled_all,
    hidden,
    pair_own,
    pair_send,
    pair_recv,
    cross_send,
    cross_recv,
    fed_send,
    fed_recv,
    load_sem,
    up_ss,
    up_rs,
    down_ss,
    down_rs,
    normed_ss,
    normed_rs,
    gate_ss,
    gate_rs,
    stat_ss,
    stat_rs,
    active_ss,
    active_rs,
    mix_ss,
    mix_rs,
    settled_ss,
    settled_rs,
    pair_ss,
    pair_rs,
    cross_ss,
    cross_rs,
    fed_ss,
    fed_rs,
):
    n = fs_count
    f = lax.axis_index("fs")
    t = lax.axis_index("tp")
    g = lax.axis_index("grp")
    side = lax.rem(t, 2)
    mate = t + 1 - 2 * side
    across = lax.rem(t + 2, n)
    rows, width = stream.shape
    own_width = width // n
    channels = value_weight.shape[1]
    half_units = up.shape[3]
    units = 2 * half_units
    bf16, f32 = jnp.bfloat16, jnp.float32

    def remote(src, dst, ss, rs, fs, tp, grp=g):
        return pltpu.make_async_remote_copy(
            src_ref=src,
            dst_ref=dst,
            send_sem=ss,
            recv_sem=rs,
            device_id={"grp": grp, "fs": fs, "tp": tp},
            device_id_type=pl.DeviceIdType.MESH,
        )

    def dot(left, right):
        return jnp.dot(left, right, preferred_element_type=f32)

    def share(block, h):
        return pl.ds(pl.multiple_of(block * units + h * half_units, 128), half_units)

    loads = []
    for h in range(2):
        loads.append(pltpu.make_async_copy(up_hbm.at[:, share(f, h)], up.at[h, f], load_sem.at[0, h]))
        loads.append(pltpu.make_async_copy(down_hbm.at[share(f, h), :], down.at[h, f], load_sem.at[1, h]))
    for load in loads:
        load.start()
    barrier = pltpu.get_barrier_semaphore()
    for a in range(n):
        for b in range(n):
            if a or b:
                pl.semaphore_signal(
                    barrier,
                    inc=1,
                    device_id={"fs": lax.rem(f + a, n), "tp": lax.rem(t + b, n)},
                    device_id_type=pl.DeviceIdType.MESH,
                )

    pl.semaphore_signal(
        barrier,
        inc=1,
        device_id={"grp": 1 - g, "fs": f, "tp": t},
        device_id_type=pl.DeviceIdType.MESH,
    )

    def peer(base, j):
        return lax.rem(base + j, n)

    waits = []

    def up_copy(to, at):
        return remote(up_hbm.at[:, share(to, g)], up.at[g, at], up_ss.at[0, to], up_rs.at[0, at], to, t)

    def down_copy(to, at):
        return remote(down_hbm.at[share(to, g), :], down.at[g, at], down_ss.at[0, to], down_rs.at[0, at], to, t)

    def start(copy):
        copy.start()
        waits.append(copy)

    weights = {"u": (up_copy, up, up_ss, up_rs), "d": (down_copy, down, down_ss, down_rs)}

    def stage(index):
        for kind, step in zip(PLAN[index][::2], PLAN[index][1::2]):
            make, held, ss, rs = weights[kind.lower()]
            if kind.islower():
                start(make(peer(f, int(step)), f))
            else:
                at = peer(f, n - int(step))
                make(at, at).wait_recv()
                start(remote(held.at[g, at], held.at[g, at], ss.at[1, at], rs.at[1, at], f, t, 1 - g))

    def swap_wait(held, ss, rs):
        for j in range(1, n):
            at = peer(f, n - j)
            remote(held.at[1 - g, at], held.at[1 - g, at], ss.at[1, at], rs.at[1, at], f, t, 1 - g).wait_recv()

    half = rows // 2
    mine = pl.ds(pl.multiple_of(side * half, half), half)
    theirs = pl.ds(pl.multiple_of((1 - side) * half, half), half)

    def normed_copy(to, at):
        return remote(
            normed_send.at[to, mine], normed_all.at[at, mine], normed_ss.at[0, to], normed_rs.at[0, at], to, t
        )

    def normed_pass(at, part):
        return remote(
            normed_all.at[at, part], normed_all.at[at, part], normed_ss.at[1, at], normed_rs.at[1, at], f, mate
        )

    pl.semaphore_wait(barrier, n * n)
    stage(0)

    def norm_in(i, carry):
        at = pl.ds(pl.multiple_of(i * 16, 16), 16)
        normed = norm_rows(stream[at, :].astype(f32), in_gain[...]).astype(bf16)
        for a in range(n):
            normed_send[a, at, :] = normed[:, a * own_width : (a + 1) * own_width]
        return carry

    lax.fori_loop(0, rows // 16, norm_in, 0)

    for j in range(1, n):
        start(normed_copy(peer(f, j), f))
    stage(1)
    normed_all[f] = normed_send[f]
    for j in range(1, n):
        at = peer(f, j)
        normed_copy(at, at).wait_recv()
        start(normed_pass(at, mine))

    for j in range(1, n + 1):
        to = peer(f, j)
        if j < n:
            normed_pass(to, theirs).wait_recv()
        values = dot(normed_all[to], value_weight[...])
        gating = dot(normed_all[to], gate_weight[...])
        if j < n:
            gate_send[to, :, :channels] = values.astype(bf16)
            gate_send[to, :, channels:] = gating.astype(bf16)
            copy = remote(gate_send.at[to], gate_recv.at[f], gate_ss.at[to], gate_rs.at[f], to, t)
            copy.start()
            waits.append(copy)
    stage(2)
    for j in range(1, n):
        at = peer(f, j)
        remote(gate_send.at[at], gate_recv.at[at], gate_ss.at[at], gate_rs.at[at], at, t).wait_recv()
        got = gate_recv[at].astype(f32)
        values = values + got[:, :channels]
        gating = gating + got[:, channels:]
    gated = (values * jax.nn.sigmoid(gating)).astype(bf16).astype(f32)

    taps = conv_kernel.shape[0]
    pad = padded.shape[1] - seq_length
    pieces = []
    for s in range(rows // seq_length):
        padded[s, :pad, :] = jnp.zeros((pad, channels), f32)
        padded[s, pad:, :] = gated[s * seq_length : (s + 1) * seq_length]
        total = jnp.zeros((seq_length, channels), f32)
        for k in range(taps):
            begin = pad - (taps - 1) + k
            total = total + padded[s, begin : begin + seq_length, :] * conv_kernel[k : k + 1, :].astype(f32)
        pieces.append(total)
    convolved = pieces[0] if len(pieces) == 1 else jnp.concatenate(pieces, axis=0)

    def shared_sums(which, values, axis, then=None):
        sums = jnp.sum(values, axis=1, keepdims=True)
        squares = jnp.sum(values * values, axis=1, keepdims=True)
        mine = to_rows(sums, squares)
        stat_send[which] = mine
        me = f if axis == "fs" else t
        for j in range(1, n):
            to = peer(me, j)
            copy = remote(
                stat_send.at[which],
                stat_recv.at[which, me],
                stat_ss.at[which, to],
                stat_rs.at[which, me],
                to if axis == "fs" else f,
                to if axis == "tp" else t,
            )
            copy.start()
            waits.append(copy)
        if then is not None:
            stage(then)
        for j in range(1, n):
            at = peer(me, j)
            remote(
                stat_send.at[which],
                stat_recv.at[which, at],
                stat_ss.at[which, at],
                stat_rs.at[which, at],
                at if axis == "fs" else f,
                at if axis == "tp" else t,
            ).wait_recv()
            mine = mine + stat_recv[which, at]
        return from_rows(mine)

    sums, squares = shared_sums(0, convolved, "tp", 3)
    activated = jax.nn.silu(
        normalize(convolved, sums, squares, channels * n, conv_gain[...]) + conv_shift[...]
    ).astype(bf16)
    active_all[f] = activated
    for j in range(1, n):
        to = peer(f, j)
        start(remote(active_all.at[f], active_all.at[f], active_ss.at[to], active_rs.at[f], to, t))
    stage(4)

    for j in range(1, n + 1):
        at = peer(t, j)

        @pl.when(at != f)
        def _():
            remote(active_all.at[at], active_all.at[at], active_ss.at[at], active_rs.at[at], at, t).wait_recv()

        mix_send[at] = dot(active_all[at], out_weight[...]).astype(bf16)
        if j < n:
            copy = remote(mix_send.at[at], mix_recv.at[t], mix_ss.at[at], mix_rs.at[t], f, at)
            copy.start()
            waits.append(copy)
    stage(5)
    mixed = mix_send[t].astype(f32)
    for j in range(1, n):
        at = peer(t, j)
        remote(mix_send.at[at], mix_recv.at[at], mix_ss.at[at], mix_rs.at[at], f, at).wait_recv()
        mixed = mixed + mix_recv[at].astype(f32)
    summed = residual_scale * normed_all[t].astype(f32) + mixed.astype(bf16).astype(f32)
    sums, squares = shared_sums(1, summed, "fs", 6)
    gain_own = norm_gain[:, pl.ds(pl.multiple_of(f * own_width, 128), own_width)]
    settled_all[t, f] = normalize(summed, sums, squares, width, gain_own).astype(bf16)

    def settled_copy(step, group, block, fs, tp, key=None):
        where = settled_all.at[group, block]
        send = block if key is None else key
        return remote(where, where, settled_ss.at[step, send], settled_rs.at[step, block], fs, tp)

    for j in range(1, n):
        start(settled_copy(0, t, f, peer(f, j), t, peer(f, j)))
    stage(7)
    for j in range(n):
        at = peer(f, j)
        if j > 0:
            settled_copy(0, t, at, at, t).wait_recv()
        start(settled_copy(1, t, at, f, across))
        start(settled_copy(2, t, at, f, mate))
    for j in range(n):
        at = peer(f, j)
        settled_copy(1, across, at, f, across).wait_recv()
        start(settled_copy(3, across, at, f, mate))
    stage(8)
    for load in loads:
        load.wait()
    swap_wait(up, up_ss, up_rs)

    def make_hidden(group):
        for h in range(2):
            total = jnp.zeros((rows, half_units), f32)
            for b in range(n):
                total = total + dot(settled_all[group, b], up[h, b])
            hidden[group, h] = jnp.square(jnp.maximum(total, 0.0)).astype(bf16)

    make_hidden(t)
    stage(9)
    for j in range(n):
        at = peer(f, j)
        settled_copy(2, mate, at, f, mate).wait_recv()
    make_hidden(mate)
    make_hidden(across)
    opposite = lax.rem(mate + 2, n)
    for j in range(n):
        at = peer(f, j)
        settled_copy(3, opposite, at, f, mate).wait_recv()
    make_hidden(opposite)
    stage(10)
    swap_wait(down, down_ss, down_rs)

    def fed_part(group, block):
        return dot(hidden[group, 0], down[0, block]) + dot(hidden[group, 1], down[1, block])

    def pair_copy(r):
        return remote(pair_send.at[r], pair_recv.at[r], pair_ss.at[r], pair_rs.at[r], f, mate)

    def cross_copy(r):
        return remote(cross_send.at[r], cross_recv.at[r], cross_ss.at[r], cross_rs.at[r], f, across)

    for j in range(1, n + 1):
        r = peer(f, j)
        pair_send[r, 0] = fed_part(r, mate).astype(bf16)
        pair_send[r, 1] = fed_part(r, opposite).astype(bf16)
        start(pair_copy(r))
        pair_own[r, 0] = fed_part(r, t)
        pair_own[r, 1] = fed_part(r, across)
        pair_copy(r).wait_recv()
        pair_own[r, 0] += pair_recv[r, 0].astype(f32)
        cross_send[r] = (pair_own[r, 1] + pair_recv[r, 1].astype(f32)).astype(bf16)
        start(cross_copy(r))
    for j in range(1, n + 1):
        r = peer(f, j)
        cross_copy(r).wait_recv()
        fed = pair_own[r, 0] + cross_recv[r].astype(f32)
        if j < n:
            fed_send[r] = fed.astype(bf16)
            start(remote(fed_send.at[r], fed_recv.at[f], fed_ss.at[r], fed_rs.at[f], r, t))
    for j in range(1, n):
        at = peer(f, j)
        remote(fed_send.at[at], fed_recv.at[at], fed_ss.at[at], fed_rs.at[at], at, t).wait_recv()
        fed = fed + fed_recv[at].astype(f32)
    final = residual_scale * settled_all[f, t].astype(f32) + fed.astype(bf16).astype(f32)
    sums, squares = shared_sums(2, final, "tp")
    out[...] = normalize(final, sums, squares, width, out_gain[...]).astype(bf16)
    for copy in waits:
        copy.wait_send()


def fast_shards(
    stream,
    in_gain,
    value_weight,
    gate_weight,
    conv_kernel,
    conv_gain,
    conv_shift,
    out_weight,
    norm_gain,
    up_weight,
    down_weight,
    out_gain,
):
    seq_count, seq_length, width = stream.shape
    rows = seq_count * seq_length
    n = lax.axis_size("fs")
    own = width // n
    channels = value_weight.shape[1]
    units = up_weight.shape[1]
    half_units = units // n // 2
    taps = conv_kernel.shape[0]
    pad = -(-(taps - 1) // 8) * 8
    bf16, f32 = jnp.bfloat16, jnp.float32
    vmem, dma = pltpu.VMEM, pltpu.SemaphoreType.DMA
    whole = pl.BlockSpec(memory_space=pltpu.VMEM)
    far = pl.BlockSpec(memory_space=pl.ANY)
    result = pl.pallas_call(
        functools.partial(layer_kernel, n, seq_length),
        out_shape=jax.ShapeDtypeStruct((rows, own), bf16),
        in_specs=[whole] * 9 + [far, far, whole],
        out_specs=whole,
        scratch_shapes=[
            vmem((2, n, own, half_units), bf16),
            vmem((2, n, half_units, own), bf16),
            vmem((n, rows, own), bf16),
            vmem((n, rows, own), bf16),
            vmem((n, rows, 2 * channels), bf16),
            vmem((n, rows, 2 * channels), bf16),
            vmem((seq_count, pad + seq_length, channels), f32),
            vmem((3, 8, rows), f32),
            vmem((3, n, 8, rows), f32),
            vmem((n, rows, channels), bf16),
            vmem((n, rows, own), bf16),
            vmem((n, rows, own), bf16),
            vmem((n, n, rows, own), bf16),
            vmem((n, 2, rows, half_units), bf16),
            vmem((n, 2, rows, own), f32),
            vmem((n, 2, rows, own), bf16),
            vmem((n, 2, rows, own), bf16),
            vmem((n, rows, own), bf16),
            vmem((n, rows, own), bf16),
            vmem((n, rows, own), bf16),
            vmem((n, rows, own), bf16),
            dma((2, 2)),
            dma((2, n)),
            dma((2, n)),
            dma((2, n)),
            dma((2, n)),
            dma((2, n)),
            dma((2, n)),
            dma((n,)),
            dma((n,)),
            dma((3, n)),
            dma((3, n)),
            dma((n,)),
            dma((n,)),
            dma((n,)),
            dma((n,)),
            dma((4, n)),
            dma((4, n)),
            dma((n,)),
            dma((n,)),
            dma((n,)),
            dma((n,)),
            dma((n,)),
            dma((n,)),
        ],
        compiler_params=pltpu.CompilerParams(
            collective_id=0, has_side_effects=True, vmem_limit_bytes=60 * 1024 * 1024
        ),
    )(
        stream.reshape(rows, width),
        in_gain[None],
        value_weight,
        gate_weight,
        conv_kernel,
        conv_gain[None],
        conv_shift[None],
        out_weight,
        norm_gain[None],
        up_weight,
        down_weight,
        out_gain[None],
    )
    return result.reshape(seq_count, seq_length, own)


def layer(*args):
    stream, value_weight, up_weight = args[0], args[2], args[9]
    n = lax.axis_size("fs")
    fits = (
        n == lax.axis_size("tp")
        and n == 4
        and lax.axis_size("grp") == 2
        and stream.shape[0] * stream.shape[1] == 128
        and stream.shape[1] % 8 == 0
        and stream.shape[2] % (128 * n) == 0
        and value_weight.shape[1] % 128 == 0
        and up_weight.shape[1] % (256 * n) == 0
    )
    return fast_shards(*args) if fits else shards(*args)


def solution(mesh):
    in_specs = (
        P(("grp", "fs"), None, None),
        P(),
        P("fs", "tp"),
        P("fs", "tp"),
        P(None, "tp"),
        P("tp"),
        P("tp"),
        P("tp", "fs"),
        P(),
        P("fs", "tp"),
        P("tp", "fs"),
        P("tp"),
    )
    out_specs = P(("grp", "fs"), None, "tp")
    return jax.shard_map(layer, mesh=mesh, in_specs=in_specs, out_specs=out_specs, check_vma=False)
```
